32 devices in a mesh: rep: 2 (over x), fs: 8 (over z, y), tp: 2 (over core).
Axes of the slice: x: 2, y: 2, z: 4, core: 2. Of those that a mesh axis runs over, the one named last changes fastest.
Arguments:
- residual: bfloat16 [16, 384, 2048], P(('rep', 'fs'), None, 'tp'), may hold values from -6 to 6
- gain_first: float32 [2048], replicated, may hold values from 0.1 to 1.9
- gain_mixer: float32 [2048], replicated, may hold values from 0.1 to 1.9
- gain_last: float32 [2048], replicated, may hold values from 0.1 to 1.9
- hidden_gate: float32 [2048, 6144], P('fs', 'tp'), may hold values from -0.125 to 0.125
- hidden_up: float32 [2048, 6144], P('fs', 'tp'), may hold values from -0.125 to 0.125
- hidden_down: float32 [6144, 2048], P('tp', 'fs'), may hold values from -0.078125 to 0.078125
- gate_scale: float32 [6144], replicated, may hold values from 0.5 to 2
- up_scale: float32 [6144], replicated, may hold values from 0.5 to 2
- down_scale: float32 [2048], replicated, may hold values from 0.5 to 2
- mix_value: float32 [2048, 2048], P('fs', 'tp'), may hold values from -0.125 to 0.125
- mix_gate: float32 [2048, 2048], P('fs', 'tp'), may hold values from -0.125 to 0.125
- value_scale: float32 [2048], replicated, may hold values from 0.5 to 2
- gating_scale: float32 [2048], replicated, may hold values from 0.5 to 2
- mix_taps: float32 [31, 2048], replicated, may hold values from -1.25 to 1.25
- mix_gain: float32 [2048], replicated, may hold values from 0.1 to 1.9
- mix_out: float32 [2048, 2048], P('tp', 'fs'), may hold values from -0.125 to 0.125
- out_scale: float32 [2048], replicated, may hold values from 0.5 to 2
Outputs:
- updated: bfloat16 [16, 384, 2048], P(('rep', 'fs'), None, 'tp')
The draws below stay inside these ranges and needn't reach their ends.
All inputs are finite; a program needn't handle non-finite values.
Results may differ from the reference program's by a relative error of at most 0.024.
Values may be sent and summed in bfloat16 or wider, within the bound.
A program may use at most 128 MiB of HBM per device.

```python
import math
import jax
import jax.numpy as jnp
from jax import lax

D = 2048
FF = 6144
KW = 31
SEQ = 384
SEQS = 16
N_TP = 2


def draw_mix_taps(key, part):
    channel = jnp.arange(D).astype(jnp.float32) / max(D - 1, 1)
    base = jnp.clip(jax.random.normal(key, (KW, D), jnp.float32), -4.0, 4.0)
    ramp = jnp.power(3.0, channel) / jnp.sqrt(3.0)
    return (base * ramp[None, :] * KW ** (-0.5)).astype(jnp.float32)


def steps_of(key, shape, cuts, least, top_value):
    def one(dim, blocks):
        draws = jax.random.uniform(jax.random.fold_in(jax.random.fold_in(key, 6), dim), (blocks,), jnp.float32, least / len(cuts), top_value / len(cuts))
        return jnp.repeat(jnp.exp(draws), shape[dim] // blocks).reshape((-1,) + (1,) * (len(shape) - dim - 1))

    factor_of = one(*cuts[0])
    for cut in cuts[1:]:
        factor_of = factor_of * one(*cut)
    return factor_of


def gaussian(stream_key, shape, deviation, limit, cuts=(), kind=jnp.bfloat16):
    loudness = steps_of(stream_key, shape, cuts, -0.22, 0.18) if cuts else 1.0
    array = jax.random.normal(stream_key, shape, jnp.float32) * deviation * loudness
    return jnp.minimum(jnp.maximum(array, -limit), limit).astype(kind)


def setup_inputs(seed: int = 0) -> dict:
    streams_of = jax.random.split(jax.random.key(seed), 19)
    residual = gaussian(streams_of[0], (SEQS, SEQ, D), 1.0, 6.0, ((0, 16), (2, 2)))
    gain_first = jnp.clip(1.0 + 0.18 * jax.random.normal(streams_of[1], (D,), jnp.float32), 0.1, 1.9)
    gain_mixer = jnp.clip(1.0 + 0.18 * jax.random.normal(streams_of[2], (D,), jnp.float32), 0.1, 1.9)
    gain_last = jnp.clip(1.0 + 0.18 * jax.random.normal(streams_of[3], (D,), jnp.float32), 0.1, 1.9)
    hidden_gate = gaussian(streams_of[4], (D, FF), D ** -0.5, 0.125, ((0, 8), (1, 2)), jnp.float32)
    hidden_up = gaussian(streams_of[5], (D, FF), D ** -0.5, 0.125, ((0, 8), (1, 2)), jnp.float32)
    hidden_down = gaussian(streams_of[6], (FF, D), FF ** -0.5, 0.078125, ((0, 2), (1, 8)), jnp.float32)
    gate_scale = jnp.clip(jnp.exp(jax.random.uniform(streams_of[7], (FF,), jnp.float32, math.log(0.5), math.log(2.0))), 0.5, 2.0)
    up_scale = jnp.clip(jnp.exp(jax.random.uniform(streams_of[8], (FF,), jnp.float32, math.log(0.5), math.log(2.0))), 0.5, 2.0)
    down_scale = jnp.clip(jnp.exp(jax.random.uniform(streams_of[9], (D,), jnp.float32, math.log(0.5), math.log(2.0))), 0.5, 2.0)
    mix_value = gaussian(streams_of[10], (D, D), D ** -0.5, 0.125, ((0, 8), (1, 2)), jnp.float32)
    mix_gate = gaussian(streams_of[11], (D, D), D ** -0.5, 0.125, ((0, 8), (1, 2)), jnp.float32)
    value_scale = jnp.clip(jnp.exp(jax.random.uniform(streams_of[12], (D,), jnp.float32, math.log(0.5), math.log(2.0))), 0.5, 2.0)
    gating_scale = jnp.clip(jnp.exp(jax.random.uniform(streams_of[13], (D,), jnp.float32, math.log(0.5), math.log(2.0))), 0.5, 2.0)
    mix_taps = draw_mix_taps(jax.random.fold_in(streams_of[18], 71), 0)
    mix_gain = jnp.clip(1.0 + 0.18 * jax.random.normal(streams_of[15], (D,), jnp.float32), 0.1, 1.9)
    mix_out = gaussian(streams_of[16], (D, D), D ** -0.5, 0.125, ((0, 2), (1, 8)), jnp.float32)
    out_scale = jnp.clip(jnp.exp(jax.random.uniform(streams_of[17], (D,), jnp.float32, math.log(0.5), math.log(2.0))), 0.5, 2.0)
    return dict(residual=residual, gain_first=gain_first, gain_mixer=gain_mixer, gain_last=gain_last, hidden_gate=hidden_gate, hidden_up=hidden_up, hidden_down=hidden_down, gate_scale=gate_scale, up_scale=up_scale, down_scale=down_scale, mix_value=mix_value, mix_gate=mix_gate, value_scale=value_scale, gating_scale=gating_scale, mix_taps=mix_taps, mix_gain=mix_gain, mix_out=mix_out, out_scale=out_scale)


EPS = 1e-06

def normalize(stream, gain):
    values = stream.astype(jnp.float32)
    scaled = values * lax.rsqrt(lax.optimization_barrier(jnp.mean(values * values, axis=-1, keepdims=True)) + EPS) * gain
    return scaled.astype(jnp.bfloat16)

def block_sum(left, weight, scale):
    blocks = left.shape[1] // N_TP
    total = jnp.zeros((left.shape[0], weight.shape[1]), jnp.float32)
    for index in range(N_TP):
        piece = jnp.dot(left[:, index * blocks:(index + 1) * blocks], weight[index * blocks:(index + 1) * blocks], preferred_element_type=jnp.float32) * scale
        total = total + lax.optimization_barrier(piece.astype(jnp.bfloat16)).astype(jnp.float32)
    return total

def inner_half(stream, gain, gate_w, up_w, down_w, gate_scale, up_scale, down_scale):
    normed = normalize(stream, gain)
    gate = jnp.dot(normed, gate_w, preferred_element_type=jnp.float32) * gate_scale
    upward = jnp.dot(normed, up_w, preferred_element_type=jnp.float32) * up_scale
    hidden = (jax.nn.silu(gate) * upward).astype(jnp.bfloat16)
    return block_sum(hidden, down_w, down_scale)

def mixer(stream, gain, value_w, gate_w, value_scale, gating_scale, taps, mix_gain, out_w, out_scale):
    normed = normalize(stream, gain)
    value = jnp.dot(normed, value_w, preferred_element_type=jnp.float32) * value_scale
    gating = jnp.dot(normed, gate_w, preferred_element_type=jnp.float32) * gating_scale
    glu = lax.optimization_barrier((value * jax.nn.sigmoid(gating)).astype(jnp.bfloat16)).astype(jnp.float32)
    length = glu.shape[0]
    span = taps.shape[0]
    padded = jnp.pad(glu, ((span - 1, 0), (0, 0)))
    wave = jnp.zeros_like(glu)
    for offset in range(span):
        wave = wave + taps[offset] * padded[span - 1 - offset:span - 1 - offset + length]
    acted = jax.nn.silu(wave * lax.rsqrt(lax.optimization_barrier(jnp.mean(wave * wave, axis=-1, keepdims=True)) + EPS) * mix_gain).astype(jnp.bfloat16)
    return block_sum(acted, out_w, out_scale)

def reference(residual, gain_first, gain_mixer, gain_last, hidden_gate, hidden_up, hidden_down, gate_scale, up_scale, down_scale, mix_value, mix_gate, value_scale, gating_scale, mix_taps, mix_gain, mix_out, out_scale):
    gate_w = hidden_gate.astype(jnp.bfloat16)
    up_w = hidden_up.astype(jnp.bfloat16)
    down_w = hidden_down.astype(jnp.bfloat16)
    value_w = mix_value.astype(jnp.bfloat16)
    mgate_w = mix_gate.astype(jnp.bfloat16)
    out_w = mix_out.astype(jnp.bfloat16)

    def one_sequence(stream):
        first = (stream.astype(jnp.float32) + 0.5 * inner_half(stream, gain_first, gate_w, up_w, down_w, gate_scale, up_scale, down_scale)).astype(jnp.bfloat16)
        second = (first.astype(jnp.float32) + mixer(first, gain_mixer, value_w, mgate_w, value_scale, gating_scale, mix_taps, mix_gain, out_w, out_scale)).astype(jnp.bfloat16)
        return (second.astype(jnp.float32) + 0.5 * inner_half(second, gain_last, gate_w, up_w, down_w, gate_scale, up_scale, down_scale)).astype(jnp.bfloat16)
    return lax.map(one_sequence, residual)
```

```python
import jax
import jax.numpy as jnp
from jax import lax
from jax.sharding import PartitionSpec as P

EPS = 1e-06
F32 = jnp.float32
BF16 = jnp.bfloat16


def on_device(
    sizes,
    residual,
    gain_first,
    gain_mixer,
    gain_last,
    hidden_gate,
    hidden_up,
    hidden_down,
    gate_scale,
    up_scale,
    down_scale,
    mix_value,
    mix_gate,
    value_scale,
    gating_scale,
    mix_taps,
    mix_gain,
    mix_out,
    out_scale,
):
    reps, fs, tps = sizes["rep"], sizes["fs"], sizes["tp"]
    outer = 4 if fs % 4 == 0 else fs
    inner = fs // outer
    rep = lax.axis_index("rep")
    fs_rank = lax.axis_index("fs")
    tp_rank = lax.axis_index("tp")
    z, y = fs_rank // inner, fs_rank % inner
    seq_len, width_local = residual.shape[1], residual.shape[2]
    hidden_local = hidden_gate.shape[1] // reps
    chan_local = mix_value.shape[1] // reps

    def along_z(piece):
        perm = [
            (a * inner + b, ((a + 1) % outer) * inner + b)
            for a in range(outer)
            for b in range(inner)
        ]
        return lax.ppermute(piece, "fs", perm)

    def along_y(piece):
        perm = [
            (a * inner + b, a * inner + (b + 1) % inner)
            for a in range(outer)
            for b in range(inner)
        ]
        return lax.ppermute(piece, "fs", perm)

    def owner(k, j):
        return ((z - k + outer) % outer) * inner + (y - j + inner) % inner

    def gather(piece, axis, y_first):
        arrived = {(0, 0): piece}
        if y_first:
            for j in range(1, inner):
                arrived[0, j] = along_y(arrived[0, j - 1])
            for k in range(1, outer):
                for j in range(inner):
                    arrived[k, j] = along_z(arrived[k - 1, j])
        else:
            for k in range(outer):
                if k:
                    arrived[k, 0] = along_z(arrived[k - 1, 0])
                for j in range(1, inner):
                    arrived[k, j] = along_y(arrived[k, j - 1])
        shape = list(piece.shape)
        span = shape[axis]
        shape[axis] = span * fs
        whole = jnp.zeros(shape, piece.dtype)
        for (k, j), part in arrived.items():
            whole = lax.dynamic_update_slice_in_dim(whole, part, owner(k, j) * span, axis)
        return whole

    def share(matrix, axis):
        span = matrix.shape[axis] // reps
        return lax.dynamic_slice_in_dim(matrix, rep * span, span, axis).astype(BF16)

    def cols(vector, span, axis=0):
        return lax.dynamic_slice_in_dim(vector, (tp_rank * reps + rep) * span, span, axis)

    gate_w = gather(share(hidden_gate, 1), 0, False)
    up_w = gather(share(hidden_up, 1), 0, False)
    down_w = gather(share(hidden_down, 0), 1, False)
    value_w = gather(share(mix_value, 1), 0, True)
    mgate_w = gather(share(mix_gate, 1), 0, True)
    out_w = gather(share(mix_out, 0), 1, False)

    gate_cols = cols(gate_scale, hidden_local)
    up_cols = cols(up_scale, hidden_local)
    value_cols = cols(value_scale, chan_local)
    gating_cols = cols(gating_scale, chan_local)
    gain_cols = cols(mix_gain, chan_local)
    tap_cols = cols(mix_taps, chan_local, 1)

    def swap(array, axis_name):
        return lax.ppermute(array, axis_name, [(0, 1), (1, 0)])

    def collect(array, axis_name, size, rank, axis):
        if size == 1:
            return array
        if size != 2:
            return lax.all_gather(array, axis_name, axis=axis, tiled=True)
        other = swap(array, axis_name)
        low = rank == 0
        return jnp.concatenate(
            [jnp.where(low, array, other), jnp.where(low, other, array)], axis=axis
        )

    def reduce_to(array, axis_name, size, rank, axis):
        if size == 1:
            return array
        if size != 2:
            return lax.psum_scatter(
                array.astype(BF16), axis_name, scatter_dimension=axis, tiled=True
            ).astype(F32)
        half = array.shape[axis] // 2
        low = lax.slice_in_dim(array, 0, half, axis=axis)
        high = lax.slice_in_dim(array, half, 2 * half, axis=axis)
        mine = jnp.where(rank == 0, low, high)
        theirs = jnp.where(rank == 0, high, low).astype(BF16)
        return mine.astype(F32) + swap(theirs, axis_name).astype(F32)

    def normed_rows(stream, gain):
        rows = collect(stream, "rep", reps, rep, 0)
        values = collect(rows, "tp", tps, tp_rank, 1).astype(F32)
        scaled = values * lax.rsqrt(jnp.mean(values * values, axis=-1, keepdims=True) + EPS) * gain
        return scaled.astype(BF16)

    def spread_sum(left, scale, matrix):
        terms = (jnp.dot(left, matrix, preferred_element_type=F32) * scale).astype(BF16)
        part = reduce_to(terms, "tp", tps, tp_rank, 1)
        return reduce_to(part, "rep", reps, rep, 0)

    def inner_half(stream, gain):
        normed = normed_rows(stream, gain)
        gate = jnp.dot(normed, gate_w, preferred_element_type=F32) * gate_cols
        upward = jnp.dot(normed, up_w, preferred_element_type=F32) * up_cols
        hidden = (jax.nn.silu(gate) * upward).astype(BF16)
        return spread_sum(hidden, down_scale, down_w)

    stream = residual[0]
    first = (stream.astype(F32) + 0.5 * inner_half(stream, gain_first)).astype(BF16)
    normed = normed_rows(first, gain_mixer)
    value = jnp.dot(normed, value_w, preferred_element_type=F32) * value_cols
    gating = jnp.dot(normed, mgate_w, preferred_element_type=F32) * gating_cols
    glu = lax.optimization_barrier((value * jax.nn.sigmoid(gating)).astype(BF16))
    glu = glu.astype(F32).reshape(reps, seq_len, chan_local)
    span = tap_cols.shape[0]
    padded = jnp.pad(glu, ((0, 0), (span - 1, 0), (0, 0)))
    wave = jnp.zeros_like(glu)
    for offset in range(span):
        start = span - 1 - offset
        wave = wave + tap_cols[offset] * padded[:, start : start + seq_len]
    wave = wave.reshape(reps * seq_len, chan_local)
    total_sq = lax.psum(jnp.sum(wave * wave, axis=1), ("rep", "tp"))
    inverse = lax.rsqrt(total_sq / mix_taps.shape[1] + EPS)
    acted = jax.nn.silu(wave * inverse[:, None] * gain_cols).astype(BF16)
    second = (first.astype(F32) + spread_sum(acted, out_scale, out_w)).astype(BF16)
    updated = (second.astype(F32) + 0.5 * inner_half(second, gain_last)).astype(BF16)
    return updated[None]


def solution(mesh):
    sizes = dict(mesh.shape)
    in_specs = (
        P(("rep", "fs"), None, "tp"),
        P(),
        P(),
        P(),
        P("fs", "tp"),
        P("fs", "tp"),
        P("tp", "fs"),
        P(),
        P(),
        P(),
        P("fs", "tp"),
        P("fs", "tp"),
        P(),
        P(),
        P(),
        P(),
        P("tp", "fs"),
        P(),
    )
    out_specs = P(("rep", "fs"), None, "tp")

    def step(*arrays):
        return on_device(sizes, *arrays)

    return jax.shard_map(
        step, mesh=mesh, in_specs=in_specs, out_specs=out_specs, check_vma=False
    )
```

```python
import jax
import jax.numpy as jnp
from jax import lax
from jax.sharding import PartitionSpec as P

EPS = 1e-06
F32 = jnp.float32
BF16 = jnp.bfloat16


def on_device(
    sizes,
    residual,
    gain_first,
    gain_mixer,
    gain_last,
    hidden_gate,
    hidden_up,
    hidden_down,
    gate_scale,
    up_scale,
    down_scale,
    mix_value,
    mix_gate,
    value_scale,
    gating_scale,
    mix_taps,
    mix_gain,
    mix_out,
    out_scale,
):
    reps, fs, tps = sizes["rep"], sizes["fs"], sizes["tp"]
    outer = 4 if fs % 4 == 0 else fs
    inner = fs // outer
    rep = lax.axis_index("rep")
    fs_rank = lax.axis_index("fs")
    tp_rank = lax.axis_index("tp")
    z, y = fs_rank // inner, fs_rank % inner
    seq_len, width_local = residual.shape[1], residual.shape[2]
    hidden_local = hidden_gate.shape[1] // reps
    chan_local = mix_value.shape[1] // reps

    def along_z(piece):
        perm = [
            (a * inner + b, ((a + 1) % outer) * inner + b)
            for a in range(outer)
            for b in range(inner)
        ]
        return lax.ppermute(piece, "fs", perm)

    def along_y(piece):
        perm = [
            (a * inner + b, a * inner + (b + 1) % inner)
            for a in range(outer)
            for b in range(inner)
        ]
        return lax.ppermute(piece, "fs", perm)

    def owner(k, j):
        return ((z - k + outer) % outer) * inner + (y - j + inner) % inner

    def hops(piece, y_first):
        arrived = {(0, 0): piece}
        if y_first:
            for j in range(1, inner):
                arrived[0, j] = along_y(arrived[0, j - 1])
            for k in range(1, outer):
                for j in range(inner):
                    arrived[k, j] = along_z(arrived[k - 1, j])
        else:
            for k in range(outer):
                if k:
                    arrived[k, 0] = along_z(arrived[k - 1, 0])
                for j in range(1, inner):
                    arrived[k, j] = along_y(arrived[k, j - 1])
        return arrived

    def tie(*arrays):
        return lax.optimization_barrier(arrays)

    def after(piece, arrived, k):
        k = min(k, outer - 1)
        piece, arrived[k, 0] = tie(piece, arrived[k, 0])
        return piece

    def assemble(whole, arrived, axis, stride, base=0):
        for (k, j), part in arrived.items():
            whole = lax.dynamic_update_slice_in_dim(whole, part, owner(k, j) * stride + base, axis)
        return whole

    def blank(piece, axis, arrived):
        shape = list(piece.shape)
        shape[axis] *= fs
        key = (min(1, outer - 1), 0)
        zero, arrived[key] = tie(jnp.zeros((), piece.dtype), arrived[key])
        return jnp.broadcast_to(zero, shape)

    def share(matrix, axis):
        span = matrix.shape[axis] // reps
        part = lax.dynamic_slice_in_dim(matrix, rep * span, span, axis).astype(BF16)
        return lax.optimization_barrier(part)

    def cols(vector, span, axis=0):
        return lax.dynamic_slice_in_dim(vector, (tp_rank * reps + rep) * span, span, axis)

    gate_piece = share(hidden_gate, 1)
    rows = gate_piece.shape[0]
    gate_z = hops(gate_piece, False)
    up_piece = share(hidden_up, 1)
    up_z = hops(up_piece, False)
    down_piece = share(hidden_down, 0)
    down_z = hops(down_piece, False)
    value_piece = after(share(mix_value, 1), down_z, 2)
    value_z = hops(value_piece, False)
    mgate_piece = after(share(mix_gate, 1), down_z, 2)
    mgate_z = hops(mgate_piece, False)
    out_piece = after(share(mix_out, 0), down_z, 2)
    out_z = hops(out_piece, False)

    gate_w = assemble(blank(gate_piece, 0, gate_z), gate_z, 0, rows)
    up_w = assemble(blank(up_piece, 0, up_z), up_z, 0, rows)
    down_w = assemble(blank(down_piece, 1, down_z), down_z, 1, down_piece.shape[1])

    def hold(array, step):
        last = outer - 1
        if step == 0:
            keys = ((value_z, (2, 0)), (mgate_z, (2, 0)), (out_z, (2, 0)))
        else:
            keys = ((value_z, (0, inner - 1)),)
        keys = [(arrived, (min(k, last), j)) for arrived, (k, j) in keys]
        array, *rest = tie(array, *[arrived[key] for arrived, key in keys])
        for (arrived, key), value in zip(keys, rest):
            arrived[key] = value
        return array

    gate_cols = cols(gate_scale, hidden_local)
    up_cols = cols(up_scale, hidden_local)
    value_cols = cols(value_scale, chan_local)
    gating_cols = cols(gating_scale, chan_local)
    gain_cols = cols(mix_gain, chan_local)
    tap_cols = cols(mix_taps, chan_local, 1)

    def swap(array, axis_name):
        return lax.ppermute(array, axis_name, [(0, 1), (1, 0)])

    def collect(array, axis_name, size, rank, axis):
        if size == 1:
            return array
        if size != 2:
            return lax.all_gather(array, axis_name, axis=axis, tiled=True)
        other = swap(array, axis_name)
        low = rank == 0
        return jnp.concatenate(
            [jnp.where(low, array, other), jnp.where(low, other, array)], axis=axis
        )

    def reduce_to(array, axis_name, size, rank, axis):
        if size == 1:
            return array
        if size != 2:
            return lax.psum_scatter(
                array.astype(BF16), axis_name, scatter_dimension=axis, tiled=True
            ).astype(F32)
        half = array.shape[axis] // 2
        low = lax.slice_in_dim(array, 0, half, axis=axis)
        high = lax.slice_in_dim(array, half, 2 * half, axis=axis)
        mine = jnp.where(rank == 0, low, high)
        theirs = jnp.where(rank == 0, high, low).astype(BF16)
        return mine.astype(F32) + swap(theirs, axis_name).astype(F32)

    def normed_rows(stream, gain):
        rows = collect(stream, "rep", reps, rep, 0)
        values = collect(rows, "tp", tps, tp_rank, 1).astype(F32)
        scaled = values * lax.rsqrt(jnp.mean(values * values, axis=-1, keepdims=True) + EPS) * gain
        return scaled.astype(BF16)

    def spread_sum(left, scale, matrix, holds):
        if holds:
            left = hold(left, 0)
        terms = (jnp.dot(left, matrix, preferred_element_type=F32) * scale).astype(BF16)
        if holds:
            terms = hold(terms, 1)
        part = reduce_to(terms, "tp", tps, tp_rank, 1)
        return reduce_to(part, "rep", reps, rep, 0)

    def inner_half(stream, gain, holds=False):
        normed = normed_rows(stream, gain)
        gate = jnp.dot(normed, gate_w, preferred_element_type=F32) * gate_cols
        upward = jnp.dot(normed, up_w, preferred_element_type=F32) * up_cols
        hidden = lax.optimization_barrier((jax.nn.silu(gate) * upward).astype(BF16))
        return spread_sum(hidden, down_scale, down_w, holds)

    def own_and_peer(stream, gain):
        blocks = (stream, swap(stream, "rep"))
        normed = []
        for block in blocks:
            values = collect(block, "tp", tps, tp_rank, 1).astype(F32)
            mean = jnp.mean(values * values, axis=-1, keepdims=True)
            normed.append((values * lax.rsqrt(mean + EPS) * gain).astype(BF16))
        return normed

    def own_sum(own, peer, scale, matrix):
        sent = (jnp.dot(peer, matrix, preferred_element_type=F32) * scale).astype(BF16)
        sent = reduce_to(sent, "tp", tps, tp_rank, 1).astype(BF16)
        got = swap(sent, "rep")
        kept = (jnp.dot(own, matrix, preferred_element_type=F32) * scale).astype(BF16)
        return reduce_to(kept, "tp", tps, tp_rank, 1) + got.astype(F32)

    def gated(normed):
        gate = jnp.dot(normed, gate_w, preferred_element_type=F32) * gate_cols
        upward = jnp.dot(normed, up_w, preferred_element_type=F32) * up_cols
        return lax.optimization_barrier((jax.nn.silu(gate) * upward).astype(BF16))

    def last_half(stream, gain):
        if reps != 2:
            return inner_half(stream, gain)
        own, peer = own_and_peer(stream, gain)
        return own_sum(gated(own), gated(peer), down_scale, down_w)

    stream = residual[0]
    first = (stream.astype(F32) + 0.5 * inner_half(stream, gain_first, True)).astype(BF16)
    value_w = assemble(blank(value_piece, 0, value_z), value_z, 0, rows)
    mgate_w = assemble(blank(mgate_piece, 0, mgate_z), mgate_z, 0, rows)
    out_w = assemble(blank(out_piece, 1, out_z), out_z, 1, out_piece.shape[1])
    normed = normed_rows(first, gain_mixer)
    value = jnp.dot(normed, value_w, preferred_element_type=F32) * value_cols
    gating = jnp.dot(normed, mgate_w, preferred_element_type=F32) * gating_cols
    glu = lax.optimization_barrier((value * jax.nn.sigmoid(gating)).astype(BF16))
    glu = glu.astype(F32).reshape(reps, seq_len, chan_local)
    span = tap_cols.shape[0]
    padded = jnp.pad(glu, ((0, 0), (span - 1, 0), (0, 0)))
    wave = jnp.zeros_like(glu)
    for offset in range(span):
        start = span - 1 - offset
        wave = wave + tap_cols[offset] * padded[:, start : start + seq_len]
    wave = wave.reshape(reps * seq_len, chan_local)
    total_sq = lax.psum(jnp.sum(wave * wave, axis=1), ("rep", "tp"))
    inverse = lax.rsqrt(total_sq / mix_taps.shape[1] + EPS)
    acted = jax.nn.silu(wave * inverse[:, None] * gain_cols).astype(BF16)
    second = (first.astype(F32) + spread_sum(acted, out_scale, out_w, False)).astype(BF16)
    updated = (second.astype(F32) + 0.5 * last_half(second, gain_last)).astype(BF16)
    return updated[None]


def solution(mesh):
    sizes = dict(mesh.shape)
    in_specs = (
        P(("rep", "fs"), None, "tp"),
        P(),
        P(),
        P(),
        P("fs", "tp"),
        P("fs", "tp"),
        P("tp", "fs"),
        P(),
        P(),
        P(),
        P("fs", "tp"),
        P("fs", "tp"),
        P(),
        P(),
        P(),
        P(),
        P("tp", "fs"),
        P(),
    )
    out_specs = P(("rep", "fs"), None, "tp")

    def step(*arrays):
        return on_device(sizes, *arrays)

    return jax.shard_map(
        step, mesh=mesh, in_specs=in_specs, out_specs=out_specs, check_vma=False
    )
```
